32 devices in a mesh: fs: 8 (over z, y), tp: 4 (over x, core).
Axes of the slice: x: 2, y: 2, z: 4, core: 2. Of those that a mesh axis runs over, the one named last changes fastest.
Arguments:
- tokens: bfloat16 [8192, 2048], P('fs', 'tp'), may hold values from -6 to 6
- mix_gain: float32 [2048], replicated, may hold values from 0.1 to 1.9
- in_weight: float32 [2048, 1024], P('fs', 'tp'), may hold values from -0.125 to 0.125
- in_scale: float32 [1024], P('tp'), may hold values from 0.4 to 2.5
- out_weight: float32 [1024, 2048], P('tp', 'fs'), may hold values from -0.1875 to 0.1875
- out_scale: float32 [2048], P('fs'), may hold values from 0.4 to 2.5
- ffn_gain: float32 [2048], replicated, may hold values from 0.1 to 1.9
- gate_weight: float32 [2048, 6144], P('fs', 'tp'), may hold values from -0.125 to 0.125
- gate_scale: float32 [6144], P('tp'), may hold values from 0.4 to 2.5
- up_weight: float32 [2048, 6144], P('fs', 'tp'), may hold values from -0.125 to 0.125
- up_scale: float32 [6144], P('tp'), may hold values from 0.4 to 2.5
- down_weight: float32 [6144, 2048], P('tp', 'fs'), may hold values from -0.078125 to 0.078125
- down_scale: float32 [2048], P('fs'), may hold values from 0.4 to 2.5
Outputs:
- layer_out: bfloat16 [8192, 2048], P('fs', 'tp')
The draws below stay inside these ranges and needn't reach their ends.
All inputs are finite; a program needn't handle non-finite values.
Results may differ from the reference program's by a relative error of at most 0.023.
Values may be sent and summed in bfloat16 or wider, within the bound.
A program may use at most 128 MiB of HBM per device.

```python
import math
import jax
import jax.numpy as jnp
from jax import lax

D = 2048
PW = 1024
FF = 6144
GROUPS = 4
GRID_W = 64
ROWS = 16
TOKENS = 8192
GC = 256
PW_DEV = 256
FF_DEV = 1536


def levels(key, shape, cuts, smallest, top_value):
    loudness = 1.0
    for axis_at, blocks in cuts:
        steps = jax.random.uniform(jax.random.fold_in(jax.random.fold_in(key, 6), axis_at), (blocks,), jnp.float32, smallest / len(cuts), top_value / len(cuts))
        loudness = loudness * jnp.repeat(jnp.exp(steps), shape[axis_at] // blocks).reshape((-1,) + (1,) * (len(shape) - 1 - axis_at))
    return loudness


def centred(stream_key, dims, width, most, split=(), kind=jnp.bfloat16):
    level = levels(stream_key, dims, split, -0.22, 0.18) if split else 1.0
    result = jax.random.normal(stream_key, dims, jnp.float32) * width * level
    return jnp.minimum(jnp.maximum(result, -most), most).astype(kind)


def setup_inputs(seed: int = 0) -> dict:
    splits = jax.random.split(jax.random.key(seed), 14)
    return {
        "tokens": centred(splits[0], (TOKENS, D), 1.0, 6.0, ((0, 8), (1, 4))),
        "mix_gain": jnp.clip(1.0 + 0.18 * jax.random.normal(splits[1], (D,), jnp.float32), 0.1, 1.9),
        "in_weight": centred(splits[2], (D, PW), D ** -0.5, 0.125, ((0, 8), (1, 4)), jnp.float32),
        "in_scale": jnp.clip(jnp.exp(math.log(2.5) - 1.8325814 * jax.random.uniform(splits[3], (PW,), jnp.float32) ** levels(splits[3], (PW,), ((0, 4),), -0.2, 0.2)), 0.4, 2.5),
        "out_weight": centred(splits[4], (PW, D), PW ** -0.5, 0.1875, ((0, 4), (1, 8)), jnp.float32),
        "out_scale": jnp.clip(jnp.exp(math.log(2.5) - 1.8325814 * jax.random.uniform(splits[5], (D,), jnp.float32) ** levels(splits[5], (D,), ((0, 8),), -0.2, 0.2)), 0.4, 2.5),
        "ffn_gain": jnp.clip(1.0 + 0.18 * jax.random.normal(splits[6], (D,), jnp.float32), 0.1, 1.9),
        "gate_weight": centred(splits[7], (D, FF), D ** -0.5, 0.125, ((0, 8), (1, 4)), jnp.float32),
        "gate_scale": jnp.clip(jnp.exp(math.log(2.5) - 1.8325814 * jax.random.uniform(splits[8], (FF,), jnp.float32) ** levels(splits[8], (FF,), ((0, 4),), -0.2, 0.2)), 0.4, 2.5),
        "up_weight": centred(splits[9], (D, FF), D ** -0.5, 0.125, ((0, 8), (1, 4)), jnp.float32),
        "up_scale": jnp.clip(jnp.exp(math.log(2.5) - 1.8325814 * jax.random.uniform(splits[10], (FF,), jnp.float32) ** levels(splits[10], (FF,), ((0, 4),), -0.2, 0.2)), 0.4, 2.5),
        "down_weight": centred(splits[11], (FF, D), FF ** -0.5, 0.078125, ((0, 4), (1, 8)), jnp.float32),
        "down_scale": jnp.clip(jnp.exp(math.log(2.5) - 1.8325814 * jax.random.uniform(splits[12], (D,), jnp.float32) ** levels(splits[12], (D,), ((0, 8),), -0.2, 0.2)), 0.4, 2.5),
    }


WINDOWS = (2, 4, 8, 16)
EPSILON = 1e-06

def box_mean(values, window, along):
    length = values.shape[along]
    position = jnp.arange(length, dtype=jnp.int32)
    lower_end = jnp.clip(position - window // 2, 0, length).astype(jnp.int32)
    upper_end = jnp.clip(position + (window - window // 2), 0, length).astype(jnp.int32)
    padding = [(0, 0)] * values.ndim
    padding[along] = (1, 0)
    running = jnp.pad(jnp.cumsum(values, axis=along), padding)
    summed = jnp.take(running, upper_end, axis=along) - jnp.take(running, lower_end, axis=along)
    shaped = [1] * values.ndim
    shaped[along] = length
    return summed / (upper_end - lower_end).astype(jnp.float32).reshape(shaped)

def norm_input(stream, gain):
    inverse_rms = lax.rsqrt(lax.optimization_barrier(jnp.mean(stream * stream, axis=-1, keepdims=True)) + EPSILON)
    return ((stream * gain).astype(jnp.bfloat16), inverse_rms)

def block_sum(hidden, weight, scale, extent):
    total = jnp.zeros((hidden.shape[0], weight.shape[1]), jnp.float32)
    for member in range(hidden.shape[1] // extent):
        term = jnp.dot(hidden[:, member * extent:(member + 1) * extent], weight[member * extent:(member + 1) * extent], preferred_element_type=jnp.float32) * scale
        total = total + term.astype(jnp.bfloat16).astype(jnp.float32)
    return total

def reference(tokens, mix_gain, in_weight, in_scale, out_weight, out_scale, ffn_gain, gate_weight, gate_scale, up_weight, up_scale, down_weight, down_scale):
    stream = tokens.astype(jnp.float32)
    normed, inverse_rms = norm_input(stream, mix_gain)
    channels = jnp.dot(normed, in_weight.astype(jnp.bfloat16), preferred_element_type=jnp.float32) * inverse_rms * in_scale
    lattice = channels.reshape(-1, ROWS, GRID_W, GROUPS, GC)
    differences = []
    for group in range(GROUPS):
        values = lattice[:, :, :, group]
        smoothed = box_mean(box_mean(values, WINDOWS[group], 2), WINDOWS[group], 1)
        differences.append(smoothed - values)
    pooled = jnp.stack(differences, axis=3).reshape(TOKENS, PW).astype(jnp.bfloat16)
    mixed = block_sum(pooled, out_weight.astype(jnp.bfloat16), out_scale, PW_DEV)
    residual = (stream + mixed).astype(jnp.bfloat16)
    normed_ffn, inverse_ffn = norm_input(residual.astype(jnp.float32), ffn_gain)
    gate_value = jnp.dot(normed_ffn, gate_weight.astype(jnp.bfloat16), preferred_element_type=jnp.float32) * inverse_ffn * gate_scale
    up_value = jnp.dot(normed_ffn, up_weight.astype(jnp.bfloat16), preferred_element_type=jnp.float32) * inverse_ffn * up_scale
    hidden = (jax.nn.silu(gate_value) * up_value).astype(jnp.bfloat16)
    channel_out = block_sum(hidden, down_weight.astype(jnp.bfloat16), down_scale, FF_DEV)
    return (residual.astype(jnp.float32) + channel_out).astype(jnp.bfloat16)
```

```python
import jax
import jax.numpy as jnp
from jax import lax
from jax.sharding import PartitionSpec as P

GROUPS = 4
GRID_W = 64
GC = 256
WINDOWS = (2, 4, 8, 16)
EPSILON = 1e-06


def box_matrix(length, window):
    position = jnp.arange(length, dtype=jnp.int32)
    lower_end = jnp.clip(position - window // 2, 0, length)
    upper_end = jnp.clip(position + (window - window // 2), 0, length)
    inside = (position[None, :] >= lower_end[:, None]) & (position[None, :] < upper_end[:, None])
    return inside.astype(jnp.float32) / (upper_end - lower_end).astype(jnp.float32)[:, None]


def smooth(lattice, window):
    across = jnp.einsum(
        "jk,akc->ajc", box_matrix(GRID_W, window), lattice, precision=lax.Precision.HIGHEST
    )
    return jnp.einsum(
        "ab,bjc->ajc",
        box_matrix(lattice.shape[0], window),
        across,
        precision=lax.Precision.HIGHEST,
    )


def pooled_differences(channels, channel_offset):
    tokens_here, extent = channels.shape
    lattice = channels.reshape(tokens_here // GRID_W, GRID_W, extent)
    if GC % extent == 0:
        result = smooth(lattice, jnp.asarray(WINDOWS, jnp.int32)[channel_offset // GC])
    else:
        group_of = (channel_offset + jnp.arange(extent, dtype=jnp.int32)) // GC
        result = jnp.zeros_like(lattice)
        for group in range(GROUPS):
            result = jnp.where(
                (group_of == group)[None, None, :], smooth(lattice, WINDOWS[group]), result
            )
    return (result - lattice).reshape(tokens_here, extent).astype(jnp.bfloat16)


class Grid:
    def __init__(self, fs, tp):
        self.ys = max(tp // 2, 1)
        self.zs = fs // self.ys
        index = lax.axis_index("fs")
        self.z, self.y = index // self.ys, index % self.ys

    def gather(self, block):
        rows = []
        for s in range(self.zs):
            pairs = [
                (z * self.ys + y, (z + s) % self.zs * self.ys + y)
                for z in range(self.zs)
                for y in range(self.ys)
            ]
            rows.append(lax.ppermute(block, "fs", pairs) if s else block)
        found = []
        for s, row in enumerate(rows):
            for t in range(self.ys):
                pairs = [
                    (z * self.ys + y, z * self.ys + (y + t) % self.ys)
                    for z in range(self.zs)
                    for y in range(self.ys)
                ]
                item = lax.ppermute(row, "fs", pairs) if t else row
                index = lax.rem(self.z - s + self.zs, self.zs) * self.ys + lax.rem(
                    self.y - t + self.ys, self.ys
                )
                found.append((index, item))
        return found


def stack(pieces):
    shape = (len(pieces),) + pieces[0][1].shape
    result = jnp.zeros(shape, pieces[0][1].dtype)
    for index, item in pieces:
        result = lax.dynamic_update_index_in_dim(result, item, index, 0)
    return result


def rows_of(pieces):
    whole = stack(pieces)
    return whole.reshape(whole.shape[0] * whole.shape[1], whole.shape[2])


def fold_rows(features, gain, weights):
    widened = lax.all_gather(features, "tp", axis=1, tiled=True)
    widened = widened.astype(jnp.float32)
    inverse_rms = lax.rsqrt(jnp.mean(widened * widened, axis=1) + EPSILON)[:, None]
    scaled = (widened * gain).astype(jnp.bfloat16)
    return tuple(
        jnp.dot(scaled, weight, preferred_element_type=jnp.float32) * inverse_rms
        for weight in weights
    )


def column_product(hidden, pieces):
    terms = stack(
        [
            (index, jnp.dot(hidden, item, preferred_element_type=jnp.float32).astype(jnp.bfloat16))
            for index, item in pieces
        ]
    )
    mine = lax.psum_scatter(terms, "tp", scatter_dimension=0, tiled=True)
    return mine.transpose(1, 0, 2).reshape(hidden.shape[0], -1).astype(jnp.float32)


def low(weight, scale=None):
    weight = weight.astype(jnp.bfloat16)
    if scale is None:
        return weight
    return (weight.astype(jnp.float32) * scale).astype(jnp.bfloat16)


def solution(mesh):
    fs, tp = mesh.shape["fs"], mesh.shape["tp"]

    def layer(
        tokens,
        mix_gain,
        in_weight,
        in_scale,
        out_weight,
        out_scale,
        ffn_gain,
        gate_weight,
        gate_scale,
        up_weight,
        up_scale,
        down_weight,
        down_scale,
    ):
        grid = Grid(fs, tp)
        wide = gate_weight.shape[1]
        both_pieces = grid.gather(jnp.concatenate([low(gate_weight), low(up_weight)], axis=1))
        down_pieces = grid.gather(low(down_weight, down_scale))
        small = lax.all_gather(
            jnp.stack([low(in_weight), low(out_weight, out_scale)]), "fs", axis=0
        )
        in_full = small[:, 0].reshape(-1, in_weight.shape[1])
        out_pieces = [(j, small[j, 1]) for j in range(fs)]
        (channels,) = fold_rows(tokens, mix_gain, (in_full,))
        channels = channels * in_scale
        pooled = pooled_differences(channels, lax.axis_index("tp") * channels.shape[1])
        mixed = column_product(pooled, out_pieces)
        residual = (tokens.astype(jnp.float32) + mixed).astype(jnp.bfloat16)
        (both,) = fold_rows(residual, ffn_gain, (rows_of(both_pieces),))
        gate_value = both[:, :wide] * gate_scale
        up_value = both[:, wide:] * up_scale
        hidden = (jax.nn.silu(gate_value) * up_value).astype(jnp.bfloat16)
        channel_out = column_product(hidden, down_pieces)
        return (residual.astype(jnp.float32) + channel_out).astype(jnp.bfloat16)

    return jax.shard_map(
        layer,
        mesh=mesh,
        in_specs=(
            P("fs", "tp"),
            P(),
            P("fs", "tp"),
            P("tp"),
            P("tp", "fs"),
            P("fs"),
            P(),
            P("fs", "tp"),
            P("tp"),
            P("fs", "tp"),
            P("tp"),
            P("tp", "fs"),
            P("fs"),
        ),
        out_specs=P("fs", "tp"),
        check_vma=False,
    )
```
